32 devices in a mesh: sp: 4 (over y, x), tp: 8 (over z, core).
Axes of the slice: x: 2, y: 2, z: 4, core: 2. Of those that a mesh axis runs over, the one named last changes fastest.
Arguments:
- queries: bfloat16 [1536, 2048], P('sp', 'tp'), may hold values from -6 to 6
- cell_key_rows: bfloat16 [1536, 2048], P('sp', 'tp'), may hold values from -6 to 6
- cell_value_rows: bfloat16 [1536, 2048], P('sp', 'tp'), may hold values from -6 to 6
- output_gate_logits: bfloat16 [1536, 2048], P('sp', 'tp'), may hold values from -6 to 6
- input_gate_logs: float32 [16, 1536], P('tp', 'sp'), may hold values from -5 to 250
- forget_gate_logits: float32 [16, 1536], P('tp', 'sp'), may hold values from 1 to 13
- extra_log_forget: float32 [16, 1536], P('tp', 'sp'), may hold values from -0.7 to 0
- head_norm_gain: float32 [2048], P('tp'), may hold values from 0.1 to 1.9
- cell_output_matrix: bfloat16 [2048, 4096], P('tp'), may hold values from -0.125 to 0.125
- residual: bfloat16 [1536, 4096], P('sp'), may hold values from -6 to 6
- expert_norm_gain: float32 [4096], replicated, may hold values from 0.1 to 1.9
- routes: int32 [1536, 2], P('sp'), may hold values from 0 to 3, all different within a row; in each aligned block of 48 rows (0 to 47, 48 to 95, ...) at most 48 rows name the same one
- token_expert_weights: float32 [1536, 2], P('sp'), may hold values from 0.2 to 1
- expert_gate_matrix: bfloat16 [4, 4096, 2048], P('sp', None, 'tp'), may hold values from -0.09375 to 0.09375
- expert_up_matrix: bfloat16 [4, 4096, 2048], P('sp', None, 'tp'), may hold values from -0.09375 to 0.09375
- expert_down_matrix: bfloat16 [4, 2048, 4096], P('sp', 'tp'), may hold values from -0.125 to 0.125
Outputs:
- layer_out: bfloat16 [1536, 4096], P(('sp', 'tp'))
The draws below stay inside these ranges and needn't reach their ends.
Inputs may be any that keep to these rules, and one draw needn't show every extreme that they name: `routes`: each row names 2 different experts. In the rows of one device (aligned blocks of 48 rows) no expert is named more than 48 times, and in some blocks one expert is named exactly 48 times.
All inputs are finite; a program needn't handle non-finite values.
Results may differ from the reference program's by a relative error of at most 0.019.
Values may be sent and summed in bfloat16 or wider, within the bound.
A program may use at most 128 MiB of HBM per device.

```python
import math
import jax
import jax.numpy as jnp
import numpy as np
from jax import lax

D = 4096
HEADS = 16
HEAD_DIM = 128
MIX = 2048
FF = 2048
EXPERTS = 4
TOPK = 2
S_DEV = 384
SEQ = 1536
TOK_DEV = 48
CAP = 48
BLOCK = 128
N_TP = 8


def draw_forget_gate_logits(key, part):
    slow_key, shift_key, noise_key = jax.random.split(jax.random.fold_in(key, 11), 3)
    pick = jax.random.uniform(slow_key, (HEADS, 1))
    slow = pick < 0.5
    noise = 0.5 * jnp.clip(jax.random.normal(noise_key, (HEADS, SEQ)), -3.0, 3.0)
    base = jnp.where(slow, jnp.log(2.0 * SEQ), jnp.log(40.0))
    shifts = jax.random.uniform(shift_key, (HEADS, SEQ // S_DEV), minval=-1.0, maxval=1.0)
    return (base + jnp.repeat(shifts, S_DEV, axis=1) + noise).astype(jnp.float32)


def draw_input_gate_logs(key, part):
    base_key = jax.random.fold_in(jax.random.fold_in(key, 13), 0)
    values = jnp.clip(jax.random.normal(base_key, (HEADS, SEQ)), -5.0, 5.0)
    return values.astype(jnp.float32)


def draw_extra_log_forget(key, part):
    place_key, size_key = jax.random.split(jax.random.fold_in(key, 17), 2)
    planted = jax.random.uniform(place_key, (HEADS, SEQ)) < 3.0 / SEQ
    sizes = jnp.log(jax.random.uniform(size_key, (HEADS, SEQ), minval=0.5, maxval=0.8))
    return jnp.where(planted, sizes, 0.0).astype(jnp.float32)


def block_levels(stream_key, shape, shards, least, top_value):
    loudness = 1.0
    for position, shards_of in shards:
        steps = jax.random.uniform(jax.random.fold_in(jax.random.fold_in(stream_key, 6), position), (shards_of,), jnp.float32, least / len(shards), top_value / len(shards))
        loudness = loudness * jnp.repeat(jnp.exp(steps), shape[position] // shards_of).reshape((-1,) + (1,) * (len(shape) - 1 - position))
    return loudness


def assign_block(rng, own, number, rows, amount, top, most, lean):
    order = jax.random.permutation(rng, amount)
    heavy_load, usual = load_shares(amount, rows * top, most, lean, True), load_shares(amount, rows * top, most, lean, False)
    places = jnp.arange(amount)

    def named(tallies, rotation):
        used = int((tallies > 0).sum())
        fixed = max(1, used // 4)
        passed = fixed + (places - fixed + rotation * (used - fixed)) % max(1, amount - fixed)
        return jnp.zeros((amount,), jnp.int32).at[order[jnp.where(places < fixed, places, passed)]].set(jnp.asarray(tallies, jnp.int32))

    tallies = jnp.where(number % 4 == 0, named(heavy_load, number // 4), named(usual, number - number // 4 - 1))
    mixed = jax.random.permutation(jax.random.fold_in(own, 3), amount)
    giver, sink = mixed[0:amount // 2 * 2:2], mixed[1:amount // 2 * 2:2]
    slack = jnp.minimum(tallies[giver] - 1, most - tallies[sink]) // 2
    slack = jnp.where((giver == order[0]) | (sink == order[0]) | (tallies[sink] == 0), 0, jnp.maximum(slack, 0))
    passed = jax.random.randint(jax.random.fold_in(own, 4), (amount // 2,), 0, 1 << 20) % (slack + 1)
    tallies = tallies.at[giver].add(-passed).at[sink].add(passed)
    items = jnp.searchsorted(jnp.cumsum(tallies), jnp.arange(rows * top), side="right").astype(jnp.int32)
    listing = items.reshape(top, rows).T
    listing = listing[jax.random.permutation(jax.random.fold_in(own, 1), rows)]
    rotation = jax.random.randint(jax.random.fold_in(own, 2), (rows, 1), 0, top)
    return jnp.take_along_axis(listing, (jnp.arange(top)[None, :] + rotation) % top, axis=1)


def load_shares(number_of, total, most, slope, full):
    weights = [(1 << 20) // math.isqrt(rank ** slope) + 1 for rank in range(1, number_of + 1)]
    largest = most if full else min(most, max(-(-total // number_of), total * weights[0] // sum(weights)))
    least = 1 if total - largest >= number_of - 1 else 0
    given, rest = [largest] + [least] * (number_of - 1), total - largest - least * (number_of - 1)
    while rest > 0:
        movable = [i for i in range(1, number_of) if given[i] < largest] or [i for i in range(1, number_of) if given[i] < most]
        mass, left = sum([weights[i] for i in movable]), rest
        for i in movable:
            more = min(most - given[i], max(1, left * weights[i] // mass), rest)
            given[i] = given[i] + more
            rest = rest - more
    return np.array(given)


def centred(stream_key, extent, scale, reach, shards=(), held_as=jnp.bfloat16):
    loudness = block_levels(stream_key, extent, shards, -0.22, 0.18) if shards else 1.0
    drawn = jax.random.normal(stream_key, extent, jnp.float32) * scale * loudness
    return jnp.minimum(jnp.maximum(drawn, -reach), reach).astype(held_as)


def setup_inputs(seed: int = 0) -> dict:
    key_list = jax.random.split(jax.random.key(seed), 17)
    queries = centred(key_list[0], (SEQ, MIX), 1.0, 6.0, ((0, 4), (1, 8)))
    cell_key_rows = centred(key_list[1], (SEQ, MIX), 1.0, 6.0, ((0, 4), (1, 8)))
    cell_value_rows = centred(key_list[2], (SEQ, MIX), 1.0, 6.0, ((0, 4), (1, 8)))
    output_gate_logits = centred(key_list[3], (SEQ, MIX), 1.0, 6.0, ((0, 4), (1, 8)))
    input_gate_logs = draw_input_gate_logs(jax.random.fold_in(key_list[16], 71), 0)
    forget_gate_logits = draw_forget_gate_logits(jax.random.fold_in(key_list[16], 71), 0)
    extra_log_forget = draw_extra_log_forget(jax.random.fold_in(key_list[16], 71), 0)
    head_norm_gain = jnp.clip(1.0 + 0.18 * jax.random.normal(key_list[7], (MIX,), jnp.float32), 0.1, 1.9)
    cell_output_matrix = centred(key_list[8], (MIX, D), MIX ** -0.5, 0.125, ((0, 8),))
    residual = centred(key_list[9], (SEQ, D), 1.0, 6.0, ((0, 4),))
    expert_norm_gain = jnp.clip(1.0 + 0.18 * jax.random.normal(key_list[10], (D,), jnp.float32), 0.1, 1.9)
    routes_keys = jax.random.split(jax.random.fold_in(key_list[11], 1), SEQ // TOK_DEV)
    routes_turns = jax.random.permutation(jax.random.fold_in(key_list[11], 3), SEQ // TOK_DEV)
    routes = jax.vmap(lambda own, number: assign_block(jax.random.fold_in(key_list[11], 2), own, number, TOK_DEV, EXPERTS, TOPK, CAP, 2))(routes_keys, routes_turns).reshape((SEQ, TOPK))
    token_expert_weights = jnp.clip(jnp.exp(math.log(1.0) - 1.609438 * jax.random.uniform(key_list[12], (SEQ, TOPK), jnp.float32) ** block_levels(key_list[12], (SEQ, TOPK), ((0, 4),), -0.2, 0.2)), 0.2, 1.0)
    expert_gate_matrix = centred(key_list[13], (EXPERTS, D, FF), D ** -0.5, 0.09375, ((0, 4), (2, 8)))
    expert_up_matrix = centred(key_list[14], (EXPERTS, D, FF), D ** -0.5, 0.09375, ((0, 4), (2, 8)))
    expert_down_matrix = centred(key_list[15], (EXPERTS, FF, D), FF ** -0.5, 0.125, ((0, 4), (1, 8)))
    return dict(queries=queries, cell_key_rows=cell_key_rows, cell_value_rows=cell_value_rows, output_gate_logits=output_gate_logits, input_gate_logs=input_gate_logs, forget_gate_logits=forget_gate_logits, extra_log_forget=extra_log_forget, head_norm_gain=head_norm_gain, cell_output_matrix=cell_output_matrix, residual=residual, expert_norm_gain=expert_norm_gain, routes=routes, token_expert_weights=token_expert_weights, expert_gate_matrix=expert_gate_matrix, expert_up_matrix=expert_up_matrix, expert_down_matrix=expert_down_matrix)


floor_neg = -1e+30
norm_eps = 1e-06
row_group = 128

def block_cells(query_f, key_f, value_f, input_f, forget_log_values, start_cell, start_stab):
    heads, length, width = query_f.shape
    count = length // BLOCK
    highest = lax.Precision.HIGHEST

    def split(array):
        return jnp.moveaxis(array.reshape((heads, count, BLOCK) + array.shape[2:]), 1, 0)
    causal = jnp.tril(jnp.ones((BLOCK, BLOCK), dtype=bool))

    def advance(carry, block):
        cell, stab = carry
        qblock, kblock, vblock, iblock, fblock = block
        cumul = jnp.cumsum(fblock, axis=-1)
        total = cumul[:, -1]
        log_inner = jnp.where(causal[None], cumul[:, :, None] - cumul[:, None, :] + iblock[:, None, :], floor_neg)
        carried = cumul + stab[:, None]
        stab_row = jnp.maximum(carried, lax.optimization_barrier(jnp.max(log_inner, axis=-1)))
        scores = jnp.einsum('hld,hsd->hls', qblock, kblock, precision=highest) * jnp.exp(log_inner - stab_row[..., None])
        numer = jnp.einsum('hls,hsd->hld', scores, vblock, precision=highest) + jnp.exp(carried - stab_row)[..., None] * jnp.einsum('hld,hde->hle', qblock, cell, precision=highest)
        log_write = total[:, None] - cumul + iblock
        stab_next = jnp.maximum(total + stab, lax.optimization_barrier(jnp.max(log_write, axis=-1)))
        weights = jnp.exp(log_write - stab_next[:, None])
        cell_next = jnp.exp(total + stab - stab_next)[:, None, None] * cell + jnp.einsum('hsd,hse->hde', kblock * weights[..., None], vblock, precision=highest)
        return ((cell_next, stab_next), (numer, stab_row))
    inputs = tuple((split(array) for array in (query_f, key_f, value_f, input_f, forget_log_values)))
    unused, (numer, stab_rows) = lax.scan(advance, (start_cell, start_stab), inputs)
    numer = jnp.moveaxis(numer, 0, 1).reshape(heads, length, width)
    stab_rows = jnp.moveaxis(stab_rows, 0, 1).reshape(heads, length)
    return (numer, stab_rows)

def rms_scale(rows, gain):
    values = rows.astype(jnp.float32)
    return (values * lax.rsqrt(lax.optimization_barrier(jnp.mean(values * values, axis=-1, keepdims=True)) + norm_eps) * gain).astype(jnp.bfloat16)

def expert_outputs(moe_in, routes, expert_gate_matrix, expert_up_matrix, expert_down_matrix):
    count = SEQ * TOPK
    expert = routes.reshape(-1).astype(jnp.int32)
    owner = jnp.arange(count, dtype=jnp.int32) // TOPK
    order = jnp.argsort(expert, stable=True).astype(jnp.int32)
    sorted_expert = expert[order]
    loads = lax.optimization_barrier(jnp.sum((expert[:, None] == jnp.arange(EXPERTS, dtype=jnp.int32)[None, :]).astype(jnp.int32), axis=0))
    starts = (jnp.cumsum(loads) - loads).astype(jnp.int32)
    padded = ((loads + row_group - 1) // row_group * row_group).astype(jnp.int32)
    ends = jnp.cumsum(padded).astype(jnp.int32)
    padded_starts = ends - padded
    dest = (padded_starts[sorted_expert] + jnp.arange(count, dtype=jnp.int32) - starts[sorted_expert]).astype(jnp.int32)
    room = (count + row_group - 1) // row_group * row_group + EXPERTS * row_group
    blocks = room // row_group
    row_owner = jnp.full((room,), SEQ, jnp.int32).at[dest].set(owner[order])
    block_first = jnp.arange(blocks, dtype=jnp.int32) * row_group
    block_expert = jnp.minimum(lax.optimization_barrier(jnp.sum((block_first[:, None] >= ends[None, :]).astype(jnp.int32), axis=1)), EXPERTS - 1).astype(jnp.int32)
    padded_in = jnp.concatenate([moe_in, jnp.zeros((1, D), moe_in.dtype)], axis=0)
    block_rows = padded_in[row_owner].reshape(blocks, row_group, D)
    width = FF // N_TP

    def one_block(args):
        rows, which = args
        gate = jnp.dot(rows, expert_gate_matrix[which], preferred_element_type=jnp.float32)
        upper = jnp.dot(rows, expert_up_matrix[which], preferred_element_type=jnp.float32)
        hidden = (jax.nn.silu(gate) * upper).astype(jnp.bfloat16)
        parts = jnp.einsum('rjf,jfd->rjd', hidden.reshape(row_group, N_TP, width).astype(jnp.float32), expert_down_matrix[which].reshape(N_TP, width, D).astype(jnp.float32))
        parts = lax.optimization_barrier(parts.astype(jnp.bfloat16)).astype(jnp.float32)
        return lax.optimization_barrier(jnp.sum(parts, axis=1)).astype(jnp.bfloat16)
    outputs = lax.map(one_block, (block_rows, block_expert)).reshape(room, D)
    place = jnp.zeros((count,), jnp.int32).at[order].set(dest)
    return outputs[place].reshape(SEQ, TOPK, D)

def reference(queries, cell_key_rows, cell_value_rows, output_gate_logits, input_gate_logs, forget_gate_logits, extra_log_forget, head_norm_gain, cell_output_matrix, residual, expert_norm_gain, routes, token_expert_weights, expert_gate_matrix, expert_up_matrix, expert_down_matrix):

    def heads_of(array):
        return jnp.transpose(array.astype(jnp.float32).reshape(SEQ, HEADS, HEAD_DIM), (1, 0, 2))
    query_f = heads_of(queries)
    key_f = heads_of(cell_key_rows) * HEAD_DIM ** (-0.5)
    value_f = heads_of(cell_value_rows)
    forget_log_values = jax.nn.log_sigmoid(forget_gate_logits) + extra_log_forget
    numer, stab_rows = block_cells(query_f, key_f, value_f, input_gate_logs, forget_log_values, jnp.zeros((HEADS, HEAD_DIM, HEAD_DIM), jnp.float32), jnp.zeros((HEADS,), jnp.float32))
    scaled = numer * lax.rsqrt(lax.optimization_barrier(jnp.mean(numer * numer, axis=2, keepdims=True)) + norm_eps) * head_norm_gain.reshape(HEADS, 1, HEAD_DIM)
    mixed = jnp.transpose(scaled, (1, 0, 2)).reshape(SEQ, MIX)
    cell_out = (jax.nn.sigmoid(output_gate_logits.astype(jnp.float32)) * mixed).astype(jnp.bfloat16)
    projected = jnp.dot(cell_out, cell_output_matrix, preferred_element_type=jnp.float32)
    after_mix = (residual.astype(jnp.float32) + projected).astype(jnp.bfloat16)
    moe_in = rms_scale(after_mix, expert_norm_gain)
    chosen = expert_outputs(moe_in, routes, expert_gate_matrix, expert_up_matrix, expert_down_matrix)
    moe = lax.optimization_barrier(jnp.sum(token_expert_weights[:, :, None] * chosen.astype(jnp.float32), axis=1))
    return (after_mix.astype(jnp.float32) + moe).astype(jnp.bfloat16)
```

```python
import jax
import jax.numpy as jnp
from jax import lax
from jax.sharding import Mesh, PartitionSpec as P

HEAD_DIM = 128
floor_neg = -1e30
norm_eps = 1e-06
HIGHEST = lax.Precision.HIGHEST
F32 = jnp.float32
BF16 = jnp.bfloat16


def swap_cores(x):
    return lax.ppermute(x, "core", ((0, 1), (1, 0)))


def local(
    queries,
    cell_key_rows,
    cell_value_rows,
    output_gate_logits,
    input_gate_logs,
    forget_gate_logits,
    extra_log_forget,
    head_norm_gain,
    cell_output_matrix,
    residual,
    expert_norm_gain,
    routes,
    token_expert_weights,
    expert_gate_matrix,
    expert_up_matrix,
    expert_down_matrix,
):
    length = queries.shape[0]
    heads = queries.shape[1] // HEAD_DIM
    sp_count = lax.axis_size("sp")
    z_count = lax.axis_size("z")
    sp_index = lax.axis_index("sp")
    z_index = lax.axis_index("z")
    core = lax.axis_index("core")
    tokens = length // (z_count * 2)
    width = residual.shape[1]

    gate_own, up_own, down_own = expert_gate_matrix[0], expert_up_matrix[0], expert_down_matrix[0]
    mix_peer = swap_cores(cell_output_matrix)
    gate_peer, up_peer, down_peer = swap_cores(gate_own), swap_cores(up_own), swap_cores(down_own)

    forget_log = jax.nn.log_sigmoid(forget_gate_logits) + extra_log_forget
    running = jnp.cumsum(forget_log, axis=1)
    total = running[:, -1]
    log_write = input_gate_logs + total[:, None] - running
    stab_dev = jnp.max(log_write, axis=1)
    write = jnp.exp(log_write - stab_dev[:, None])

    def head(array, h):
        return array[:, h * HEAD_DIM : (h + 1) * HEAD_DIM]

    scale = HEAD_DIM ** (-0.5)
    cell_dev = [
        lax.dot_general(
            head(cell_key_rows, h).astype(F32) * (write[h] * scale)[:, None],
            head(cell_value_rows, h).astype(F32),
            (((0,), (0,)), ((), ())),
            precision=HIGHEST,
        )
        for h in range(heads)
    ]
    token_gates = jnp.sum(
        jnp.where(
            routes[None, :, :] == jnp.arange(sp_count, dtype=routes.dtype)[:, None, None],
            token_expert_weights[None],
            0.0,
        ),
        axis=2,
    )
    scalars = jnp.pad(jnp.concatenate([stab_dev, total])[None], ((0, 7), (0, HEAD_DIM - 2 * heads)))
    pack = jnp.concatenate(cell_dev + [scalars, token_gates.reshape(-1, HEAD_DIM)], axis=0)
    packs = lax.all_gather(pack, "sp")
    cells = packs[:, : heads * HEAD_DIM].reshape(sp_count, heads, HEAD_DIM, HEAD_DIM)
    stabs = packs[:, heads * HEAD_DIM, :heads]
    totals = packs[:, heads * HEAD_DIM, heads : 2 * heads]
    gates = packs[:, heads * HEAD_DIM + 8 :].reshape(sp_count, sp_count, length)
    gates = lax.dynamic_index_in_dim(gates, sp_index, 1, keepdims=False)

    order = jnp.arange(sp_count)
    between = (order[None, :] > order[:, None]) & (order[None, :] < sp_index)
    after = jnp.sum(jnp.where(between[:, :, None], totals[None], 0.0), axis=1)
    earlier = order < sp_index
    levels = jnp.where(earlier[:, None], stabs + after, floor_neg)
    before_total = jnp.sum(jnp.where(earlier[:, None], totals, 0.0), axis=0)
    start_stab = jnp.maximum(jnp.max(levels, axis=0), before_total)
    mixing = jnp.where(earlier[:, None], jnp.exp(levels - start_stab[None]), 0.0)
    start_cell = jnp.sum(mixing[:, :, None, None] * cells, axis=0)

    causal = jnp.tril(jnp.ones((length, length), dtype=bool))
    log_inner = jnp.where(
        causal[None],
        running[:, :, None] - running[:, None, :] + input_gate_logs[:, None, :],
        floor_neg,
    )
    inner_max = jnp.max(log_inner, axis=-1)
    carried = running + start_stab[:, None]
    stab_row = jnp.maximum(carried, inner_max)
    inner_scale = jnp.exp(inner_max - stab_row)
    carry_scale = jnp.exp(carried - stab_row)
    outs = []
    for h in range(heads):
        query = head(queries, h)
        products = lax.dot_general(
            query, head(cell_key_rows, h), (((1,), (1,)), ((), ())), preferred_element_type=F32
        )
        scores = products * (scale * jnp.exp(log_inner[h] - inner_max[h][:, None]))
        inner = jnp.dot(scores, head(cell_value_rows, h).astype(F32), precision=HIGHEST)
        carry = jnp.dot(query.astype(F32), start_cell[h], precision=HIGHEST)
        numer = inner_scale[h][:, None] * inner + carry_scale[h][:, None] * carry
        outs.append(
            numer
            * lax.rsqrt(jnp.mean(numer * numer, axis=1, keepdims=True) + norm_eps)
            * head(head_norm_gain[None], h)
        )
    cell_out = (
        jax.nn.sigmoid(output_gate_logits.astype(F32)) * jnp.concatenate(outs, axis=1)
    ).astype(BF16)

    rows = cell_out.reshape(z_count, 2, tokens, cell_out.shape[1])
    mine = lax.dynamic_index_in_dim(rows, core, 1, keepdims=False)
    theirs = swap_cores(lax.dynamic_index_in_dim(rows, 1 - core, 1, keepdims=False))
    mine = mine.reshape(z_count * tokens, -1)
    theirs = theirs.reshape(z_count * tokens, -1)
    mixed = jnp.dot(mine, cell_output_matrix, preferred_element_type=F32) + jnp.dot(
        theirs, mix_peer, preferred_element_type=F32
    )
    projected = lax.psum_scatter(mixed.astype(BF16), "z", scatter_dimension=0, tiled=True)

    start = (z_index * 2 + core) * tokens
    own_residual = lax.dynamic_slice_in_dim(residual, start, tokens, 0)
    after_mix = (own_residual.astype(F32) + projected.astype(F32)).astype(BF16)
    values = after_mix.astype(F32)
    moe_in = (
        values
        * lax.rsqrt(jnp.mean(values * values, axis=-1, keepdims=True) + norm_eps)
        * expert_norm_gain
    ).astype(BF16)

    line = lax.all_gather(moe_in, "z", axis=0, tiled=True)
    piece = lax.all_gather(line, "sp", axis=0, tiled=True)

    def hidden(gate_matrix, up_matrix):
        gate = jnp.dot(piece, gate_matrix, preferred_element_type=F32)
        upper = jnp.dot(piece, up_matrix, preferred_element_type=F32)
        return (jax.nn.silu(gate) * upper).astype(BF16)

    act = jnp.concatenate([hidden(gate_own, up_own), hidden(gate_peer, up_peer)], axis=1)
    down = jnp.concatenate([down_own, down_peer], axis=0)
    result = jnp.dot(act, down, preferred_element_type=F32)
    weight = lax.dynamic_index_in_dim(
        gates.reshape(sp_count, z_count, 2, tokens), core, 2, keepdims=False
    ).reshape(-1, 1)
    weighted = jnp.where(weight > 0, result * weight, 0.0).astype(BF16)
    summed = lax.psum_scatter(weighted, "sp", scatter_dimension=0, tiled=True)
    moe = lax.psum_scatter(summed, "z", scatter_dimension=0, tiled=True)
    return (after_mix.astype(F32) + moe.astype(F32)).astype(BF16)


def solution(mesh):
    fine = Mesh(
        mesh.devices.reshape(mesh.shape["sp"], mesh.shape["tp"] // 2, 2), ("sp", "z", "core")
    )
    tp = ("z", "core")
    placed = (
        P("sp", tp),
        P("sp", tp),
        P("sp", tp),
        P("sp", tp),
        P(tp, "sp"),
        P(tp, "sp"),
        P(tp, "sp"),
        P(tp),
        P(tp, None),
        P("sp", None),
        P(),
        P("sp", None),
        P("sp", None),
        P("sp", None, tp),
        P("sp", None, tp),
        P("sp", tp, None),
    )
    return jax.shard_map(
        local, mesh=fine, in_specs=placed, out_specs=P(("sp", "z", "core"), None), check_vma=False
    )
```

```python
import jax
import jax.numpy as jnp
from jax import lax
from jax.sharding import Mesh, PartitionSpec as P

HEAD_DIM = 128
floor_neg = -1e30
norm_eps = 1e-06
HIGHEST = lax.Precision.HIGHEST
F32 = jnp.float32
BF16 = jnp.bfloat16


def swap_cores(x):
    return lax.ppermute(x, "core", ((0, 1), (1, 0)))


def toward(x, bit):
    return lax.ppermute(x, "sp", [(i, i ^ bit) for i in range(4)])


def spread(line):
    cut = line.shape[0] // 2
    first, second = toward(line, 1), toward(line, 2)
    diagonal = jnp.concatenate([toward(first[:cut], 2), toward(second[cut:], 1)], axis=0)
    return [line, first, second, diagonal]


def collect(terms):
    own, first, second, diagonal = terms
    cut = own.shape[0] // 2

    def add(*parts):
        return sum(part.astype(F32) for part in parts).astype(BF16)

    via_first = toward(diagonal[:cut], 1)
    via_second = toward(diagonal[cut:], 2)
    first_top = toward(first[:cut], 1)
    second_low = toward(second[cut:], 2)
    second_top = toward(add(second[:cut], via_first), 2)
    first_low = toward(add(first[cut:], via_second), 1)
    top = add(own[:cut], first_top, second_top)
    low = add(own[cut:], first_low, second_low)
    return jnp.concatenate([top, low], axis=0)


def local(
    queries,
    cell_key_rows,
    cell_value_rows,
    output_gate_logits,
    input_gate_logs,
    forget_gate_logits,
    extra_log_forget,
    head_norm_gain,
    cell_output_matrix,
    residual,
    expert_norm_gain,
    routes,
    token_expert_weights,
    expert_gate_matrix,
    expert_up_matrix,
    expert_down_matrix,
):
    length = queries.shape[0]
    heads = queries.shape[1] // HEAD_DIM
    sp_count = lax.axis_size("sp")
    z_count = lax.axis_size("z")
    sp_index = lax.axis_index("sp")
    z_index = lax.axis_index("z")
    core = lax.axis_index("core")
    tokens = length // (z_count * 2)
    width = residual.shape[1]

    gate_own, up_own, down_own = expert_gate_matrix[0], expert_up_matrix[0], expert_down_matrix[0]
    mix_peer = swap_cores(cell_output_matrix)
    gate_peer, up_peer, down_peer = swap_cores(gate_own), swap_cores(up_own), swap_cores(down_own)

    forget_log = jax.nn.log_sigmoid(forget_gate_logits) + extra_log_forget
    running = jnp.cumsum(forget_log, axis=1)
    total = running[:, -1]
    log_write = input_gate_logs + total[:, None] - running
    stab_dev = jnp.max(log_write, axis=1)
    write = jnp.exp(log_write - stab_dev[:, None])

    def head(array, h):
        return array[:, h * HEAD_DIM : (h + 1) * HEAD_DIM]

    scale = HEAD_DIM ** (-0.5)
    cell_dev = [
        lax.dot_general(
            head(cell_key_rows, h).astype(F32) * (write[h] * scale)[:, None],
            head(cell_value_rows, h).astype(F32),
            (((0,), (0,)), ((), ())),
            precision=HIGHEST,
        )
        for h in range(heads)
    ]
    token_gates = jnp.sum(
        jnp.where(
            routes[None, :, :] == jnp.arange(sp_count, dtype=routes.dtype)[:, None, None],
            token_expert_weights[None],
            0.0,
        ),
        axis=2,
    )
    scalars = jnp.pad(jnp.concatenate([stab_dev, total])[None], ((0, 7), (0, HEAD_DIM - 2 * heads)))
    pack = jnp.concatenate(cell_dev + [scalars, token_gates.reshape(-1, HEAD_DIM)], axis=0)
    packs = lax.all_gather(pack, "sp")
    cells = packs[:, : heads * HEAD_DIM].reshape(sp_count, heads, HEAD_DIM, HEAD_DIM)
    stabs = packs[:, heads * HEAD_DIM, :heads]
    totals = packs[:, heads * HEAD_DIM, heads : 2 * heads]
    gates = packs[:, heads * HEAD_DIM + 8 :].reshape(sp_count, sp_count, length)
    gates = lax.dynamic_index_in_dim(gates, sp_index, 1, keepdims=False)

    order = jnp.arange(sp_count)
    between = (order[None, :] > order[:, None]) & (order[None, :] < sp_index)
    after = jnp.sum(jnp.where(between[:, :, None], totals[None], 0.0), axis=1)
    earlier = order < sp_index
    levels = jnp.where(earlier[:, None], stabs + after, floor_neg)
    before_total = jnp.sum(jnp.where(earlier[:, None], totals, 0.0), axis=0)
    start_stab = jnp.maximum(jnp.max(levels, axis=0), before_total)
    mixing = jnp.where(earlier[:, None], jnp.exp(levels - start_stab[None]), 0.0)
    start_cell = jnp.sum(mixing[:, :, None, None] * cells, axis=0)

    causal = jnp.tril(jnp.ones((length, length), dtype=bool))
    log_inner = jnp.where(
        causal[None],
        running[:, :, None] - running[:, None, :] + input_gate_logs[:, None, :],
        floor_neg,
    )
    inner_max = jnp.max(log_inner, axis=-1)
    carried = running + start_stab[:, None]
    stab_row = jnp.maximum(carried, inner_max)
    inner_scale = jnp.exp(inner_max - stab_row)
    carry_scale = jnp.exp(carried - stab_row)
    outs = []
    for h in range(heads):
        query = head(queries, h)
        products = lax.dot_general(
            query, head(cell_key_rows, h), (((1,), (1,)), ((), ())), preferred_element_type=F32
        )
        scores = products * (scale * jnp.exp(log_inner[h] - inner_max[h][:, None]))
        inner = jnp.dot(scores, head(cell_value_rows, h).astype(F32), precision=HIGHEST)
        carry = jnp.dot(query.astype(F32), start_cell[h], precision=HIGHEST)
        numer = inner_scale[h][:, None] * inner + carry_scale[h][:, None] * carry
        outs.append(
            numer
            * lax.rsqrt(jnp.mean(numer * numer, axis=1, keepdims=True) + norm_eps)
            * head(head_norm_gain[None], h)
        )
    cell_out = (
        jax.nn.sigmoid(output_gate_logits.astype(F32)) * jnp.concatenate(outs, axis=1)
    ).astype(BF16)

    rows = cell_out.reshape(z_count, 2, tokens, cell_out.shape[1])
    mine = lax.dynamic_index_in_dim(rows, core, 1, keepdims=False)
    theirs = swap_cores(lax.dynamic_index_in_dim(rows, 1 - core, 1, keepdims=False))
    mine = mine.reshape(z_count * tokens, -1)
    theirs = theirs.reshape(z_count * tokens, -1)
    mixed = jnp.dot(mine, cell_output_matrix, preferred_element_type=F32) + jnp.dot(
        theirs, mix_peer, preferred_element_type=F32
    )
    projected = lax.psum_scatter(mixed.astype(BF16), "z", scatter_dimension=0, tiled=True)

    start = (z_index * 2 + core) * tokens
    own_residual = lax.dynamic_slice_in_dim(residual, start, tokens, 0)
    after_mix = (own_residual.astype(F32) + projected.astype(F32)).astype(BF16)
    values = after_mix.astype(F32)
    moe_in = (
        values
        * lax.rsqrt(jnp.mean(values * values, axis=-1, keepdims=True) + norm_eps)
        * expert_norm_gain
    ).astype(BF16)

    weight = lax.dynamic_index_in_dim(
        gates.reshape(sp_count, z_count, 2, tokens), core, 2, keepdims=False
    ).reshape(sp_count, z_count * tokens, 1)
    square = sp_count == 4
    half = width // 2
    cuts = (slice(0, half), slice(half, width))
    pieces = []
    for cut in cuts:
        line = lax.all_gather(moe_in[:, cut], "z", axis=0, tiled=True)
        if square:
            pieces.append(spread(line))
        else:
            pieces.append([lax.all_gather(line, "sp", axis=0, tiled=True)])
    if square:
        weights = [
            lax.dynamic_index_in_dim(weight, sp_index ^ r, 0, keepdims=False) for r in range(4)
        ]
    else:
        weights = [weight.reshape(-1, 1)]

    def project(block, matrix):
        return sum(
            jnp.dot(pieces[i][block], matrix[cut], preferred_element_type=F32)
            for i, cut in enumerate(cuts)
        )

    def hidden(block, gate_matrix, up_matrix):
        gate, upper = project(block, gate_matrix), project(block, up_matrix)
        return (jax.nn.silu(gate) * upper).astype(BF16)

    acts = [
        jnp.concatenate(
            [hidden(block, gate_own, up_own), hidden(block, gate_peer, up_peer)], axis=1
        )
        for block in range(len(weights))
    ]
    down = jnp.concatenate([down_own, down_peer], axis=0)
    moe = []
    for cut in cuts:
        terms = [
            (jnp.dot(act, down[:, cut], preferred_element_type=F32) * gain).astype(BF16)
            for act, gain in zip(acts, weights)
        ]
        if square:
            summed = collect(terms)
        else:
            summed = lax.psum_scatter(terms[0], "sp", scatter_dimension=0, tiled=True)
        moe.append(lax.psum_scatter(summed, "z", scatter_dimension=0, tiled=True))
    moe = jnp.concatenate(moe, axis=1)
    return (after_mix.astype(F32) + moe.astype(F32)).astype(BF16)


def solution(mesh):
    fine = Mesh(
        mesh.devices.reshape(mesh.shape["sp"], mesh.shape["tp"] // 2, 2), ("sp", "z", "core")
    )
    tp = ("z", "core")
    placed = (
        P("sp", tp),
        P("sp", tp),
        P("sp", tp),
        P("sp", tp),
        P(tp, "sp"),
        P(tp, "sp"),
        P(tp, "sp"),
        P(tp),
        P(tp, None),
        P("sp", None),
        P(),
        P("sp", None),
        P("sp", None),
        P("sp", None, tp),
        P("sp", None, tp),
        P("sp", tp, None),
    )
    return jax.shard_map(
        local, mesh=fine, in_specs=placed, out_specs=P(("sp", "z", "core"), None), check_vma=False
    )
```
